32 devices in a mesh: ep: 4 (over y, x), tp: 8 (over z, core).
Axes of the slice: x: 2, y: 2, z: 4, core: 2. Of those that a mesh axis runs over, the one named last changes fastest.
Arguments:
- scan_source_values: bfloat16 [1024, 8192], P('tp', 'ep'), may hold values from -6 to 6
- switch_path_values: bfloat16 [1024, 8192], P('tp', 'ep'), may hold values from -6 to 6
- causal_filter_coefficients: bfloat16 [1024, 4], replicated, may hold values from -3 to 3
- scan_switch_blockmap: bfloat16 [16, 64, 64], replicated, may hold values from -0.75 to 0.75
- entry_switch_blockmap: bfloat16 [16, 64, 64], replicated, may hold values from -0.75 to 0.75
- feature_fading_speeds: float32 [1024], replicated, may hold values from 0 to 1
- spike_amount: float32 [8192], P('ep'), may hold values from -1 to 0
- final_linear_map: bfloat16 [1024, 2048], replicated, may hold values from -0.1875 to 0.1875
- dispatched_group_activity: bfloat16 [4096, 2048], P(('ep', 'tp')), may hold values from -6 to 6
- specialist_rmsgain: bfloat16 [2048], replicated, may hold values from 0.099609375 to 1.8984375
- selected_specialist_ids: int32 [4096, 2], P(('ep', 'tp')), may hold values from 0 to 3, all different within a row; in each aligned block of 128 rows (0 to 127, 128 to 255, ...) at most 96 rows name the same one
- selected_specialist_share: float32 [4096, 2], P(('ep', 'tp')), may hold values from 0.2 to 1
- specialist_switch_maps: bfloat16 [4, 2048, 2048], P('ep', None, 'tp'), may hold values from -0.3125 to 0.3125
- specialist_widen_maps: bfloat16 [4, 2048, 2048], P('ep', None, 'tp'), may hold values from -0.3125 to 0.3125
- specialist_shrink_maps: bfloat16 [4, 2048, 2048], P('ep', None, 'tp'), may hold values from -0.03125 to 0.03125
Outputs:
- scan_path_result: bfloat16 [8192, 2048], P(('ep', 'tp'))
- moe_out: bfloat16 [4096, 2048], P(('ep', 'tp'))
The draws below stay inside these ranges and needn't reach their ends.
Inputs may be any that keep to these rules, and one draw needn't show every extreme that they name: `selected_specialist_ids`: each row names 2 different experts. Among the rows of one device no expert is named more than 96 times, and in every draw some device names some expert exactly 96 times.
All inputs are finite; a program needn't handle non-finite values.
Results may differ from the reference program's by a relative error of at most 0.0085.
Values may be sent and summed in bfloat16 or wider, within the bound.
A program may use at most 128 MiB of HBM per device.

```python
import math
import jax
import jax.numpy as jnp
import numpy as np
from jax import lax

D = 2048
WIDTH = 1024
BLOCK = 64
NBLK = 16
CONV = 4
FFE = 2048
TOPK = 2
EXPERTS = 4
TOK_A = 8192
MOE_DEV = 128
TOK_B = 4096
CAP = 96


def draw_feature_fading_speeds(key, part):
    first_key, second_key, third_key = jax.random.split(key, 3)
    slow_speed = jnp.exp(jax.random.uniform(first_key, (WIDTH,), jnp.float32, math.log(0.05), math.log(0.2))) / TOK_A
    fast_speed = jnp.exp(jax.random.uniform(second_key, (WIDTH,), jnp.float32, math.log(0.003), math.log(0.01)))
    fast_share = 0.5
    chosen = jax.random.uniform(third_key, (WIDTH,), jnp.float32) < fast_share
    return jnp.where(chosen, fast_speed, slow_speed)


def draw_spike_amount(key, part):
    first_key, second_key = jax.random.split(key)
    places = jax.random.randint(first_key, (8,), 0, TOK_A)
    depth = jnp.log(jax.random.uniform(second_key, (8,), jnp.float32, 0.5, 0.8))
    matches = (jnp.arange(TOK_A, dtype=jnp.int32)[:, None] == places[None, :]).astype(jnp.float32)
    return jnp.sum(matches * depth[None, :], axis=1)


def block_levels(rng, shape, cuts, least, largest):
    def one(dim, parts):
        heights = jax.random.uniform(jax.random.fold_in(jax.random.fold_in(rng, 6), dim), (parts,), jnp.float32, least / len(cuts), largest / len(cuts))
        return jnp.repeat(jnp.exp(heights), shape[dim] // parts).reshape((-1,) + (1,) * (len(shape) - dim - 1))

    gain = one(*cuts[0])
    for cut in cuts[1:]:
        gain = gain * one(*cut)
    return gain


def shared_out(own_key, own, number, rows, count, top, most, skew):
    sequence = jax.random.permutation(own_key, count)
    packed, ordinary = load_shares(count, rows * top, most, skew, True), load_shares(count, rows * top, most, skew, False)
    places = jnp.arange(count)

    def named(tallies, offset_by):
        used = int((tallies > 0).sum())
        fixed = max(1, used // 4)
        shifted = fixed + (places - fixed + offset_by * (used - fixed)) % max(1, count - fixed)
        return jnp.zeros((count,), jnp.int32).at[sequence[jnp.where(places < fixed, places, shifted)]].set(jnp.asarray(tallies, jnp.int32))

    tallies = jnp.where(number % 4 == 0, named(packed, number // 4), named(ordinary, number - number // 4 - 1))
    mixed = jax.random.permutation(jax.random.fold_in(own, 3), count)
    giver, receiver = mixed[0:count // 2 * 2:2], mixed[1:count // 2 * 2:2]
    margin = jnp.minimum(tallies[giver] - 1, most - tallies[receiver]) // 2
    margin = jnp.where((giver == sequence[0]) | (receiver == sequence[0]) | (tallies[receiver] == 0), 0, jnp.maximum(margin, 0))
    shifted = jax.random.randint(jax.random.fold_in(own, 4), (count // 2,), 0, 1 << 20) % (margin + 1)
    tallies = tallies.at[giver].add(-shifted).at[receiver].add(shifted)
    items = jnp.searchsorted(jnp.cumsum(tallies), jnp.arange(rows * top), side="right").astype(jnp.int32)
    table = items.reshape(top, rows).T
    table = table[jax.random.permutation(jax.random.fold_in(own, 1), rows)]
    offset_by = jax.random.randint(jax.random.fold_in(own, 2), (rows, 1), 0, top)
    return jnp.take_along_axis(table, (jnp.arange(top)[None, :] + offset_by) % top, axis=1)


def load_shares(count, total, most, slope, full):
    weights = [(1 << 20) // math.isqrt(grade ** slope) + 1 for grade in range(1, count + 1)]
    largest = most if full else min(most, max(-(-total // count), total * weights[0] // sum(weights)))
    least = 1 if total - largest >= count - 1 else 0
    holding, surplus = [largest] + [least] * (count - 1), total - largest - least * (count - 1)
    while surplus > 0:
        movable = [i for i in range(1, count) if holding[i] < largest] or [i for i in range(1, count) if holding[i] < most]
        whole, remaining = sum([weights[i] for i in movable]), surplus
        for i in movable:
            addition = min(most - holding[i], max(1, remaining * weights[i] // whole), surplus)
            holding[i] = holding[i] + addition
            surplus = surplus - addition
    return np.array(holding)


def noise(stream_key, shape, spread, bound, cuts=(), kind=jnp.bfloat16):
    loudness = block_levels(stream_key, shape, cuts, -0.22, 0.18) if cuts else 1.0
    array = jax.random.normal(stream_key, shape, jnp.float32) * spread * loudness
    return jnp.minimum(jnp.maximum(array, -bound), bound).astype(kind)


def setup_inputs(seed: int = 0) -> dict:
    streams_of = jax.random.split(jax.random.key(seed), 16)
    scan_source_values = noise(streams_of[0], (WIDTH, TOK_A), 1.0, 6.0, ((0, 8), (1, 4)))
    switch_path_values = noise(streams_of[1], (WIDTH, TOK_A), 1.0, 6.0, ((0, 8), (1, 4)))
    causal_filter_coefficients = noise(streams_of[2], (WIDTH, CONV), CONV ** -0.5, 3.0)
    scan_switch_blockmap = noise(streams_of[3], (NBLK, BLOCK, BLOCK), BLOCK ** -0.5, 0.75)
    entry_switch_blockmap = noise(streams_of[4], (NBLK, BLOCK, BLOCK), BLOCK ** -0.5, 0.75)
    feature_fading_speeds = draw_feature_fading_speeds(jax.random.fold_in(streams_of[15], 71), 0)
    spike_amount = draw_spike_amount(jax.random.fold_in(streams_of[15], 71), 0)
    final_linear_map = noise(streams_of[7], (WIDTH, D), WIDTH ** -0.5, 0.1875)
    dispatched_group_activity = noise(streams_of[8], (TOK_B, D), 1.0, 6.0, ((0, 32),))
    specialist_rmsgain = jnp.clip(1.0 + 0.18 * jax.random.normal(streams_of[9], (D,), jnp.float32), 0.099609375, 1.8984375).astype(jnp.bfloat16)
    selected_specialist_ids_keys = jax.random.split(jax.random.fold_in(streams_of[10], 1), TOK_B // MOE_DEV)
    selected_specialist_ids_turns = jax.random.permutation(jax.random.fold_in(streams_of[10], 3), TOK_B // MOE_DEV)
    selected_specialist_ids = jax.vmap(lambda own, number: shared_out(jax.random.fold_in(streams_of[10], 2), own, number, MOE_DEV, EXPERTS, TOPK, CAP, 2))(selected_specialist_ids_keys, selected_specialist_ids_turns).reshape((TOK_B, TOPK))
    selected_specialist_share = jnp.clip(0.2 + 0.8 * jax.random.uniform(streams_of[11], (TOK_B, TOPK), jnp.float32) ** block_levels(streams_of[11], (TOK_B, TOPK), ((0, 32),), -0.2, 0.2), 0.2, 1.0)
    specialist_switch_maps = noise(streams_of[12], (EXPERTS, D, FFE), (D // 6) ** -0.5, 0.3125, ((0, 4), (2, 8)))
    specialist_widen_maps = noise(streams_of[13], (EXPERTS, D, FFE), (D // 6) ** -0.5, 0.3125, ((0, 4), (2, 8)))
    specialist_shrink_maps = noise(streams_of[14], (EXPERTS, D, FFE), (16 * FFE) ** -0.5, 0.03125, ((0, 4), (2, 8)))
    return {"scan_source_values": scan_source_values, "switch_path_values": switch_path_values, "causal_filter_coefficients": causal_filter_coefficients, "scan_switch_blockmap": scan_switch_blockmap, "entry_switch_blockmap": entry_switch_blockmap, "feature_fading_speeds": feature_fading_speeds, "spike_amount": spike_amount, "final_linear_map": final_linear_map, "dispatched_group_activity": dispatched_group_activity, "specialist_rmsgain": specialist_rmsgain, "selected_specialist_ids": selected_specialist_ids, "selected_specialist_share": selected_specialist_share, "specialist_switch_maps": specialist_switch_maps, "specialist_widen_maps": specialist_widen_maps, "specialist_shrink_maps": specialist_shrink_maps}


def combine_pairs(earlier, later):
    return (earlier[0] * later[0], later[0] * earlier[1] + later[1])

def scan_path(scan_source_values, switch_path_values, causal_filter_coefficients, scan_switch_blockmap, entry_switch_blockmap, feature_fading_speeds, spike_amount, final_linear_map):
    positions = scan_source_values.shape[1]
    padded = jnp.pad(scan_source_values.astype(jnp.float32), ((0, 0), (CONV - 1, 0)))
    conv_taps = causal_filter_coefficients.astype(jnp.float32)
    running = padded[:, 0:positions] * conv_taps[:, 0:1]
    for shift_tap in range(1, CONV):
        running = running + padded[:, shift_tap:shift_tap + positions] * conv_taps[:, shift_tap:shift_tap + 1]
    conv_out = running.astype(jnp.bfloat16)
    grouped = conv_out.astype(jnp.float32).reshape(NBLK, BLOCK, positions)
    scan_switch = jax.nn.sigmoid(jnp.einsum('gij,git->gjt', scan_switch_blockmap.astype(jnp.float32), grouped).reshape(WIDTH, positions))
    inflow = jax.nn.sigmoid(jnp.einsum('gij,git->gjt', entry_switch_blockmap.astype(jnp.float32), grouped).reshape(WIDTH, positions))
    fading_exponent = -8.0 * scan_switch * feature_fading_speeds[:, None] + spike_amount[None, :]
    drive = jnp.sqrt(-jnp.expm1(2.0 * fading_exponent)) * inflow * conv_out.astype(jnp.float32)
    unused, state = lax.associative_scan(combine_pairs, (jnp.exp(fading_exponent), drive), axis=1)
    mix_hidden = (state * jax.nn.gelu(switch_path_values.astype(jnp.float32), approximate=True)).astype(jnp.bfloat16)
    return jnp.dot(mix_hidden.T, final_linear_map, preferred_element_type=jnp.float32).astype(jnp.bfloat16)

def expert_branch(dispatched_group_activity, specialist_rmsgain, selected_specialist_ids, selected_specialist_share, specialist_switch_maps, specialist_widen_maps, specialist_shrink_maps):
    values = dispatched_group_activity.astype(jnp.float32)
    scale = lax.rsqrt(lax.optimization_barrier(jnp.mean(values * values, axis=1, keepdims=True)) + 1e-06)
    normed = (values * scale * specialist_rmsgain.astype(jnp.float32)).astype(jnp.bfloat16)
    token_total, route_count = selected_specialist_ids.shape
    model_width = dispatched_group_activity.shape[1]
    block_count = token_total // MOE_DEV
    flat_ids = selected_specialist_ids.reshape(block_count, MOE_DEV * route_count)
    one_hot = (flat_ids[:, :, None] == jnp.arange(EXPERTS, dtype=jnp.int32)[None, None, :]).astype(jnp.int32)
    slot_rank = lax.optimization_barrier(jnp.sum((jnp.cumsum(one_hot, axis=1) - one_hot) * one_hot, axis=2))
    owner_token = jnp.arange(block_count, dtype=jnp.int32)[:, None] * MOE_DEV + jnp.arange(MOE_DEV * route_count, dtype=jnp.int32)[None, :] // route_count
    flat_weight = selected_specialist_share.reshape(block_count, MOE_DEV * route_count)
    padded_rows = jnp.concatenate([normed, jnp.zeros((1, model_width), jnp.bfloat16)], axis=0)
    slot_total = block_count * CAP

    def one_expert(running, expert):
        mine = flat_ids == expert
        slot_index = jnp.where(mine, jnp.arange(block_count, dtype=jnp.int32)[:, None] * CAP + slot_rank, slot_total).astype(jnp.int32)
        slot_token = jnp.full((slot_total + 1,), token_total, jnp.int32).at[slot_index.reshape(-1)].set(owner_token.reshape(-1))[:slot_total]
        slot_weight = jnp.zeros((slot_total + 1,), jnp.float32).at[slot_index.reshape(-1)].set(flat_weight.reshape(-1))[:slot_total]
        rows = padded_rows[jnp.minimum(slot_token, token_total)]
        gate_pre = jnp.dot(rows, specialist_switch_maps[expert], preferred_element_type=jnp.float32)
        up_pre = jnp.dot(rows, specialist_widen_maps[expert], preferred_element_type=jnp.float32)
        gate_cut = jnp.minimum(gate_pre, 7.0)
        up_cut = jnp.clip(up_pre, -7.0, 7.0)
        units = ((up_cut + 1.0) * gate_cut * jax.nn.sigmoid(1.702 * gate_cut)).astype(jnp.bfloat16)
        result = lax.dot_general(units, specialist_shrink_maps[expert], (((1,), (1,)), ((), ())), preferred_element_type=jnp.float32).astype(jnp.bfloat16)
        running = running.at[slot_token].add(result.astype(jnp.float32) * slot_weight[:, None], mode='drop')
        return (running, None)
    running, unused = lax.scan(one_expert, jnp.zeros((token_total, model_width), jnp.float32), jnp.arange(EXPERTS, dtype=jnp.int32))
    return running.astype(jnp.bfloat16)

def reference(scan_source_values, switch_path_values, causal_filter_coefficients, scan_switch_blockmap, entry_switch_blockmap, feature_fading_speeds, spike_amount, final_linear_map, dispatched_group_activity, specialist_rmsgain, selected_specialist_ids, selected_specialist_share, specialist_switch_maps, specialist_widen_maps, specialist_shrink_maps):
    scan_path_result = scan_path(scan_source_values, switch_path_values, causal_filter_coefficients, scan_switch_blockmap, entry_switch_blockmap, feature_fading_speeds, spike_amount, final_linear_map)
    moe_out = expert_branch(dispatched_group_activity, specialist_rmsgain, selected_specialist_ids, selected_specialist_share, specialist_switch_maps, specialist_widen_maps, specialist_shrink_maps)
    return (scan_path_result, moe_out)
```

```python
import jax
import jax.numpy as jnp
from jax import lax
from jax.sharding import PartitionSpec as P

BLOCK = 64


def entering_2(x, axis, combine, identity):
    count, index = (lax.axis_size(axis), lax.axis_index(axis))
    packed = lax.all_gather(jnp.stack(x), axis)
    before = identity
    for k in range(count):
        new = combine(before, (packed[k, 0], packed[k, 1]))
        reached = k < index
        before = jax.tree.map(lambda a, b: jnp.where(reached, a, b), new, before)
    return before


def from_behind(x, axis, by):
    count = lax.axis_size(axis)
    pairs = [(i, i + by) for i in range(count) if 0 <= i + by < count]
    return lax.ppermute(x, axis, pairs)


def combine_pairs(earlier, later):
    return (earlier[0] * later[0], later[0] * earlier[1] + later[1])


def expert_units(rows, gate_piece, up_piece):
    gate_pre = jnp.dot(rows, gate_piece, preferred_element_type=jnp.float32)
    up_pre = jnp.dot(rows, up_piece, preferred_element_type=jnp.float32)
    gate_cut = jnp.minimum(gate_pre, 7.0)
    up_cut = jnp.clip(up_pre, -7.0, 7.0)
    return ((up_cut + 1.0) * gate_cut * jax.nn.sigmoid(1.702 * gate_cut)).astype(jnp.bfloat16)


def down_product(units, down_piece):
    return lax.dot_general(
        units, down_piece, (((1,), (1,)), ((), ())), preferred_element_type=jnp.float32
    )


def segment_recurrence(decay, drive):
    channels, positions = decay.shape
    span = 16
    seg_count = positions // span
    decay_split = decay.reshape(channels, seg_count, span).transpose(0, 2, 1)
    drive_split = drive.reshape(channels, seg_count, span).transpose(0, 2, 1)
    run_state = jnp.zeros((channels, seg_count), jnp.float32)
    run_decay = jnp.ones((channels, seg_count), jnp.float32)
    state_list = []
    decay_list = []
    for offset in range(span):
        run_state = decay_split[:, offset] * run_state + drive_split[:, offset]
        run_decay = run_decay * decay_split[:, offset]
        state_list.append(run_state)
        decay_list.append(run_decay)
    local_state = jnp.stack(state_list, axis=1)
    local_decay = jnp.stack(decay_list, axis=1)
    decay_upto, state_upto = lax.associative_scan(combine_pairs, (run_decay, run_state), axis=1)
    decay_before = jnp.concatenate(
        [jnp.ones((channels, 1), jnp.float32), decay_upto[:, :-1]], axis=1
    )
    state_before = jnp.concatenate(
        [jnp.zeros((channels, 1), jnp.float32), state_upto[:, :-1]], axis=1
    )
    identity = (jnp.ones((channels,), jnp.float32), jnp.zeros((channels,), jnp.float32))
    carried = entering_2((decay_upto[:, -1], state_upto[:, -1]), "ep", combine_pairs, identity)
    entering = state_before + decay_before * carried[1][:, None]
    state = local_state + local_decay * entering[:, None, :]
    return state.transpose(0, 2, 1).reshape(channels, positions)


def mixer_half(
    scan_source_values,
    switch_path_values,
    causal_filter_coefficients,
    scan_switch_blockmap,
    entry_switch_blockmap,
    feature_fading_speeds,
    spike_amount,
    final_linear_map,
):
    channels, positions = scan_source_values.shape
    tp_index = lax.axis_index("tp")
    first_chan = tp_index * channels
    conv_local = lax.dynamic_slice_in_dim(
        causal_filter_coefficients, first_chan, channels, 0
    ).astype(jnp.float32)
    tap_count = conv_local.shape[1]
    rim_cells = from_behind(scan_source_values[:, positions - tap_count + 1 :], "ep", 1)
    padded = jnp.concatenate([rim_cells, scan_source_values], axis=1).astype(jnp.float32)
    running = padded[:, 0:positions] * conv_local[:, 0:1]
    for shift_tap in range(1, tap_count):
        running = (
            running
            + padded[:, shift_tap : shift_tap + positions]
            * conv_local[:, shift_tap : shift_tap + 1]
        )
    conv_out = running.astype(jnp.bfloat16)
    block_count = channels // BLOCK
    rate_local = lax.dynamic_slice_in_dim(
        scan_switch_blockmap, tp_index * block_count, block_count, 0
    )
    input_local = lax.dynamic_slice_in_dim(
        entry_switch_blockmap, tp_index * block_count, block_count, 0
    )
    grouped = conv_out.reshape(block_count, BLOCK, positions)
    block_dims = (((1,), (1,)), ((0,), (0,)))
    scan_switch = jax.nn.sigmoid(
        lax.dot_general(
            rate_local, grouped, block_dims, preferred_element_type=jnp.float32
        ).reshape(channels, positions)
    )
    inflow = jax.nn.sigmoid(
        lax.dot_general(
            input_local, grouped, block_dims, preferred_element_type=jnp.float32
        ).reshape(channels, positions)
    )
    feature_fading = lax.dynamic_slice_in_dim(feature_fading_speeds, first_chan, channels, 0)
    fading_exponent = -8.0 * scan_switch * feature_fading[:, None] + spike_amount[None, :]
    drive = jnp.sqrt(-jnp.expm1(2.0 * fading_exponent)) * inflow * conv_out.astype(jnp.float32)
    state = segment_recurrence(jnp.exp(fading_exponent), drive)
    mix_hidden = (
        state * jax.nn.gelu(switch_path_values.astype(jnp.float32), approximate=True)
    ).astype(jnp.bfloat16)
    tp_count = lax.axis_size("tp")
    pieces = mix_hidden.reshape(channels, tp_count, positions // tp_count)
    return lax.dot_general(
        lax.all_to_all(pieces, "tp", split_axis=1, concat_axis=0, tiled=True)[:, 0, :],
        final_linear_map,
        (((0,), (0,)), ((), ())),
        preferred_element_type=jnp.float32,
    ).astype(jnp.bfloat16)


def slot_places(ids, expert_count, slot_count):
    token_count = ids.shape[0]
    experts = jnp.arange(expert_count, dtype=jnp.int32)[None, None, :]
    named = (ids[:, :, None] == experts).astype(jnp.bfloat16)
    member = jnp.sum(named.astype(jnp.float32), axis=1).astype(jnp.bfloat16)
    order = jnp.arange(token_count, dtype=jnp.int32)
    earlier = (order[None, :] < order[:, None]).astype(jnp.bfloat16)
    rank = jnp.dot(earlier, member, preferred_element_type=jnp.float32)
    own_rank = jnp.sum(named.astype(jnp.float32) * rank[:, None, :], axis=2).astype(jnp.int32)
    return ids * slot_count + own_rank


def normed_rows(activity, gain):
    values = activity.astype(jnp.float32)
    scale = lax.rsqrt(jnp.mean(values * values, axis=1, keepdims=True) + 1e-06)
    return (values * scale * gain.astype(jnp.float32)).astype(jnp.bfloat16)


def rows_in_slots(rows, places, slot_total):
    slots = jnp.arange(slot_total, dtype=jnp.int32)[:, None]
    picks = slots == places[:, 0][None, :]
    for route in range(1, places.shape[1]):
        picks = picks | (slots == places[:, route][None, :])
    return jnp.dot(
        picks.astype(jnp.bfloat16), rows, preferred_element_type=jnp.float32
    ).astype(jnp.bfloat16)


def weighted_routes(returned, places, share):
    slots = jnp.arange(returned.shape[0], dtype=jnp.int32)[None, :]
    total = None
    for route in range(places.shape[1]):
        picks = (slots == places[:, route][:, None]).astype(jnp.bfloat16)
        chosen = jnp.dot(picks, returned, preferred_element_type=jnp.float32)
        term = chosen * share[:, route][:, None]
        total = term if total is None else total + term
    return total


def over_experts(rows, expert_count):
    width = rows.shape[1]
    pieces = rows.reshape(expert_count, rows.shape[0] // expert_count, width)
    return lax.all_to_all(pieces, "ep", split_axis=0, concat_axis=0, tiled=True).reshape(-1, width)


def expert_half(
    dispatched_group_activity,
    specialist_rmsgain,
    selected_specialist_ids,
    selected_specialist_share,
    specialist_switch_maps,
    specialist_widen_maps,
    specialist_shrink_maps,
):
    token_count, model_width = dispatched_group_activity.shape
    route_count = selected_specialist_ids.shape[1]
    expert_count = lax.axis_size("ep")
    slot_count = 3 * route_count * token_count // (2 * expert_count)
    slot_total = expert_count * slot_count
    tp_count = lax.axis_size("tp")
    half = tp_count // 2
    swap = [(i, (i + half) % tp_count) for i in range(tp_count)]
    halves = [list(range(half)), list(range(half, tp_count))]

    def gather_half(piece):
        return lax.all_gather(piece, "tp", axis=1, tiled=True, axis_index_groups=halves)

    table = jnp.concatenate(
        [selected_specialist_ids.astype(jnp.float32), selected_specialist_share], axis=1
    )
    far_table = lax.ppermute(table, "tp", swap)
    far_activity = lax.ppermute(dispatched_group_activity, "tp", swap)
    gate_full = gather_half(specialist_switch_maps[0])
    up_full = gather_half(specialist_widen_maps[0])
    down_full = gather_half(specialist_shrink_maps[0])

    near_places = slot_places(selected_specialist_ids, expert_count, slot_count)
    near_rows = rows_in_slots(
        normed_rows(dispatched_group_activity, specialist_rmsgain), near_places, slot_total
    )
    near_arrived = over_experts(near_rows, expert_count)
    far_ids = far_table[:, :route_count].astype(jnp.int32)
    far_share = far_table[:, route_count:]
    far_places = slot_places(far_ids, expert_count, slot_count)
    far_rows = rows_in_slots(
        normed_rows(far_activity, specialist_rmsgain), far_places, slot_total
    )
    far_arrived = over_experts(far_rows, expert_count)
    arrived = jnp.concatenate([far_arrived, near_arrived], axis=0)
    units = expert_units(arrived, gate_full, up_full)
    far_result = down_product(units[:slot_total], down_full).astype(jnp.bfloat16)
    far_returned = over_experts(far_result, expert_count)
    near_result = down_product(units[slot_total:], down_full).astype(jnp.bfloat16)
    near_returned = over_experts(near_result, expert_count)
    far_sum = weighted_routes(far_returned, far_places, far_share).astype(jnp.bfloat16)
    home_sum = lax.ppermute(far_sum, "tp", swap)
    near_sum = weighted_routes(near_returned, near_places, selected_specialist_share)
    return (near_sum + home_sum.astype(jnp.float32)).astype(jnp.bfloat16)


def on_device(
    scan_source_values,
    switch_path_values,
    causal_filter_coefficients,
    scan_switch_blockmap,
    entry_switch_blockmap,
    feature_fading_speeds,
    spike_amount,
    final_linear_map,
    dispatched_group_activity,
    specialist_rmsgain,
    selected_specialist_ids,
    selected_specialist_share,
    specialist_switch_maps,
    specialist_widen_maps,
    specialist_shrink_maps,
):
    scan_path_result = mixer_half(
        scan_source_values,
        switch_path_values,
        causal_filter_coefficients,
        scan_switch_blockmap,
        entry_switch_blockmap,
        feature_fading_speeds,
        spike_amount,
        final_linear_map,
    )
    moe_out = expert_half(
        dispatched_group_activity,
        specialist_rmsgain,
        selected_specialist_ids,
        selected_specialist_share,
        specialist_switch_maps,
        specialist_widen_maps,
        specialist_shrink_maps,
    )
    return (scan_path_result, moe_out)


def solution(mesh):
    in_specs = (
        P("tp", "ep"),
        P("tp", "ep"),
        P(),
        P(),
        P(),
        P(),
        P("ep"),
        P(),
        P(("ep", "tp"), None),
        P(),
        P(("ep", "tp"), None),
        P(("ep", "tp"), None),
        P("ep", None, "tp"),
        P("ep", None, "tp"),
        P("ep", None, "tp"),
    )
    out_specs = (P(("ep", "tp"), None), P(("ep", "tp"), None))
    return jax.shard_map(
        on_device, mesh=mesh, in_specs=in_specs, out_specs=out_specs, check_vma=False
    )
```

```python
import jax
import jax.numpy as jnp
from jax import lax
from jax.experimental import pallas as pl
from jax.experimental.pallas import tpu as pltpu
from jax.sharding import PartitionSpec as P

BLOCK = 64
LANES = 128


def entering_2(x, axis, combine, identity):
    count, index = (lax.axis_size(axis), lax.axis_index(axis))
    packed = lax.all_gather(jnp.stack(x), axis)
    before = identity
    for k in range(count):
        new = combine(before, (packed[k, 0], packed[k, 1]))
        reached = k < index
        before = jax.tree.map(lambda a, b: jnp.where(reached, a, b), new, before)
    return before


def from_behind(x, axis, by):
    count = lax.axis_size(axis)
    pairs = [(i, i + by) for i in range(count) if 0 <= i + by < count]
    return lax.ppermute(x, axis, pairs)


def combine_pairs(earlier, later):
    return (earlier[0] * later[0], later[0] * earlier[1] + later[1])


def expert_units(rows, gate_piece, up_piece):
    gate_pre = jnp.dot(rows, gate_piece, preferred_element_type=jnp.float32)
    up_pre = jnp.dot(rows, up_piece, preferred_element_type=jnp.float32)
    gate_cut = jnp.minimum(gate_pre, 7.0)
    up_cut = jnp.clip(up_pre, -7.0, 7.0)
    return ((up_cut + 1.0) * gate_cut * jax.nn.sigmoid(1.702 * gate_cut)).astype(jnp.bfloat16)


def down_product(units, down_pieces):
    total = None
    for part, piece in zip(units, down_pieces):
        term = lax.dot_general(
            part, piece, (((1,), (1,)), ((), ())), preferred_element_type=jnp.float32
        )
        total = term if total is None else total + term
    return total.astype(jnp.bfloat16)


def minus_expm1(v):
    series = 1.0 + v * (1.0 / 9.0)
    for n in range(8, 1, -1):
        series = 1.0 + v * (1.0 / n) * series
    return jnp.where(v > -0.5, -v * series, 1.0 - jnp.exp(v))


def mixer_kernel(
    behind_ref, source_ref, taps_ref, maps_ref, speeds_ref, spike_ref, state_ref, decay_ref
):
    channels, positions = source_ref.shape
    tap_count = taps_ref.shape[1]
    lane = lax.broadcasted_iota(jnp.int32, (channels, LANES), 1)

    def tile(index, carry):
        before, decay_in, state_in = carry
        here = pl.ds(pl.multiple_of(index * LANES, LANES), LANES)
        values = source_ref[:, here].astype(jnp.float32)
        running = None
        for tap in range(tap_count):
            back = tap_count - 1 - tap
            moved = values
            if back:
                moved = jnp.where(
                    lane >= back, pltpu.roll(values, back, 1), pltpu.roll(before, back, 1)
                )
            term = moved * taps_ref[:, tap : tap + 1]
            running = term if running is None else running + term
        conv_out = running.astype(jnp.bfloat16)
        both = jnp.dot(maps_ref[...], conv_out, preferred_element_type=jnp.float32)
        rate = 1.0 / (1.0 + jnp.exp(-both[:channels]))
        inflow = 1.0 / (1.0 + jnp.exp(-both[channels:]))
        exponent = -8.0 * rate * speeds_ref[...] + spike_ref[:, here]
        state = jnp.sqrt(minus_expm1(2.0 * exponent)) * inflow * conv_out.astype(jnp.float32)
        decay = jnp.exp(exponent)
        step = 1
        while step < LANES:
            inside = lane >= step
            state = decay * jnp.where(inside, pltpu.roll(state, step, 1), 0.0) + state
            decay = decay * jnp.where(inside, pltpu.roll(decay, step, 1), 1.0)
            step *= 2
        state = state + decay * state_in
        decay = decay * decay_in
        state_ref[:, here] = state
        decay_ref[:, here] = decay
        return values, decay[:, LANES - 1 :], state[:, LANES - 1 :]

    start = (
        behind_ref[...].astype(jnp.float32),
        jnp.ones((channels, 1), jnp.float32),
        jnp.zeros((channels, 1), jnp.float32),
    )
    lax.fori_loop(0, positions // LANES, tile, start)


def block_diagonal(maps):
    count, rows, columns = maps.shape
    same = jnp.eye(count, dtype=maps.dtype)
    spread = maps.transpose(0, 2, 1)[:, :, None, :] * same[:, None, :, None]
    return spread.reshape(count * columns, count * rows)


def mixer_half(
    scan_source_values,
    switch_path_values,
    causal_filter_coefficients,
    scan_switch_blockmap,
    entry_switch_blockmap,
    feature_fading_speeds,
    spike_amount,
    final_linear_map,
):
    channels, positions = scan_source_values.shape
    tp_index = lax.axis_index("tp")
    first_chan = tp_index * channels
    taps = lax.dynamic_slice_in_dim(causal_filter_coefficients, first_chan, channels, 0).astype(
        jnp.float32
    )
    behind = from_behind(scan_source_values[:, positions - LANES :], "ep", 1)
    block_count = channels // BLOCK
    maps = jnp.concatenate(
        [
            block_diagonal(lax.dynamic_slice_in_dim(m, tp_index * block_count, block_count, 0))
            for m in (scan_switch_blockmap, entry_switch_blockmap)
        ],
        axis=0,
    )
    speeds = lax.dynamic_slice_in_dim(feature_fading_speeds, first_chan, channels, 0)
    whole = jax.ShapeDtypeStruct((channels, positions), jnp.float32)
    local_state, local_decay = pl.pallas_call(
        mixer_kernel,
        out_shape=(whole, whole),
        in_specs=[pl.BlockSpec(memory_space=pltpu.VMEM)] * 6,
        out_specs=[pl.BlockSpec(memory_space=pltpu.VMEM)] * 2,
        compiler_params=pltpu.CompilerParams(vmem_limit_bytes=16 * 1024 * 1024),
        cost_estimate=pl.CostEstimate(
            flops=400 * channels * positions,
            bytes_accessed=10 * channels * positions,
            transcendentals=0,
        ),
    )(behind, scan_source_values, taps, maps, speeds[:, None], spike_amount[None, :])
    identity = (jnp.ones((channels,), jnp.float32), jnp.zeros((channels,), jnp.float32))
    carried = entering_2((local_decay[:, -1], local_state[:, -1]), "ep", combine_pairs, identity)
    state = local_state + local_decay * carried[1][:, None]
    mix_hidden = (
        state * jax.nn.gelu(switch_path_values.astype(jnp.float32), approximate=True)
    ).astype(jnp.bfloat16)
    tp_count = lax.axis_size("tp")
    pieces = mix_hidden.reshape(channels, tp_count, positions // tp_count)
    return lax.dot_general(
        lax.all_to_all(pieces, "tp", split_axis=1, concat_axis=0, tiled=True)[:, 0, :],
        final_linear_map,
        (((0,), (0,)), ((), ())),
        preferred_element_type=jnp.float32,
    ).astype(jnp.bfloat16)


def slot_places(ids, expert_count, slot_count):
    token_count = ids.shape[0]
    experts = jnp.arange(expert_count, dtype=jnp.int32)[None, None, :]
    named = (ids[:, :, None] == experts).astype(jnp.bfloat16)
    member = jnp.sum(named.astype(jnp.float32), axis=1).astype(jnp.bfloat16)
    order = jnp.arange(token_count, dtype=jnp.int32)
    earlier = (order[None, :] < order[:, None]).astype(jnp.bfloat16)
    rank = jnp.dot(earlier, member, preferred_element_type=jnp.float32)
    own_rank = jnp.sum(named.astype(jnp.float32) * rank[:, None, :], axis=2).astype(jnp.int32)
    return ids * slot_count + own_rank


def normed_rows(activity, gain):
    values = activity.astype(jnp.float32)
    scale = lax.rsqrt(jnp.mean(values * values, axis=1, keepdims=True) + 1e-06)
    return (values * scale * gain.astype(jnp.float32)).astype(jnp.bfloat16)


def rows_in_slots(rows, places, slot_total):
    slots = jnp.arange(slot_total, dtype=jnp.int32)[:, None]
    picks = slots == places[:, 0][None, :]
    for route in range(1, places.shape[1]):
        picks = picks | (slots == places[:, route][None, :])
    return jnp.dot(
        picks.astype(jnp.bfloat16), rows, preferred_element_type=jnp.float32
    ).astype(jnp.bfloat16)


def weighted_routes(returned, places, share):
    slots = jnp.arange(returned.shape[0], dtype=jnp.int32)[None, :]
    total = None
    for route in range(places.shape[1]):
        picks = (slots == places[:, route][:, None]).astype(jnp.bfloat16)
        chosen = jnp.dot(picks, returned, preferred_element_type=jnp.float32)
        term = chosen * share[:, route][:, None]
        total = term if total is None else total + term
    return total


def over_experts(rows, expert_count):
    width = rows.shape[1]
    pieces = rows.reshape(expert_count, rows.shape[0] // expert_count, width)
    return lax.all_to_all(pieces, "ep", split_axis=0, concat_axis=0, tiled=True).reshape(-1, width)


def expert_half(
    dispatched_group_activity,
    specialist_rmsgain,
    selected_specialist_ids,
    selected_specialist_share,
    specialist_switch_maps,
    specialist_widen_maps,
    specialist_shrink_maps,
):
    token_count, model_width = dispatched_group_activity.shape
    route_count = selected_specialist_ids.shape[1]
    expert_count = lax.axis_size("ep")
    slot_count = 3 * route_count * token_count // (2 * expert_count)
    slot_total = expert_count * slot_count
    tp_count = lax.axis_size("tp")
    half = tp_count // 2
    swap = [(i, (i + half) % tp_count) for i in range(tp_count)]

    def half_pieces(piece):
        bit = half // 2
        while bit:
            other = lax.ppermute(piece, "tp", [(i, i ^ bit) for i in range(tp_count)])
            if bit == 1:
                return [piece, other]
            piece = jnp.concatenate([piece, other], axis=1)
            bit //= 2
        return [piece]

    table = jnp.concatenate(
        [selected_specialist_ids.astype(jnp.float32), selected_specialist_share], axis=1
    )
    far_table = lax.ppermute(table, "tp", swap)
    far_activity = lax.ppermute(dispatched_group_activity, "tp", swap)
    gate_pieces = half_pieces(specialist_switch_maps[0])
    up_pieces = half_pieces(specialist_widen_maps[0])
    down_pieces = half_pieces(specialist_shrink_maps[0])

    near_places = slot_places(selected_specialist_ids, expert_count, slot_count)
    near_rows = rows_in_slots(
        normed_rows(dispatched_group_activity, specialist_rmsgain), near_places, slot_total
    )
    near_arrived = over_experts(near_rows, expert_count)
    far_ids = far_table[:, :route_count].astype(jnp.int32)
    far_share = far_table[:, route_count:]
    far_places = slot_places(far_ids, expert_count, slot_count)
    far_rows = rows_in_slots(
        normed_rows(far_activity, specialist_rmsgain), far_places, slot_total
    )
    far_arrived = over_experts(far_rows, expert_count)
    arrived = jnp.concatenate([far_arrived, near_arrived], axis=0)
    units = [expert_units(arrived, g, u) for g, u in zip(gate_pieces, up_pieces)]
    far_result = down_product([part[:slot_total] for part in units], down_pieces)
    far_returned = over_experts(far_result, expert_count)
    near_result = down_product([part[slot_total:] for part in units], down_pieces)
    near_returned = over_experts(near_result, expert_count)
    far_sum = weighted_routes(far_returned, far_places, far_share).astype(jnp.bfloat16)
    home_sum = lax.ppermute(far_sum, "tp", swap)
    near_sum = weighted_routes(near_returned, near_places, selected_specialist_share)
    return (near_sum + home_sum.astype(jnp.float32)).astype(jnp.bfloat16)


def on_device(
    scan_source_values,
    switch_path_values,
    causal_filter_coefficients,
    scan_switch_blockmap,
    entry_switch_blockmap,
    feature_fading_speeds,
    spike_amount,
    final_linear_map,
    dispatched_group_activity,
    specialist_rmsgain,
    selected_specialist_ids,
    selected_specialist_share,
    specialist_switch_maps,
    specialist_widen_maps,
    specialist_shrink_maps,
):
    scan_path_result = mixer_half(
        scan_source_values,
        switch_path_values,
        causal_filter_coefficients,
        scan_switch_blockmap,
        entry_switch_blockmap,
        feature_fading_speeds,
        spike_amount,
        final_linear_map,
    )
    moe_out = expert_half(
        dispatched_group_activity,
        specialist_rmsgain,
        selected_specialist_ids,
        selected_specialist_share,
        specialist_switch_maps,
        specialist_widen_maps,
        specialist_shrink_maps,
    )
    return (scan_path_result, moe_out)


def solution(mesh):
    in_specs = (
        P("tp", "ep"),
        P("tp", "ep"),
        P(),
        P(),
        P(),
        P(),
        P("ep"),
        P(),
        P(("ep", "tp"), None),
        P(),
        P(("ep", "tp"), None),
        P(("ep", "tp"), None),
        P("ep", None, "tp"),
        P("ep", None, "tp"),
        P("ep", None, "tp"),
    )
    out_specs = (P(("ep", "tp"), None), P(("ep", "tp"), None))
    return jax.shard_map(
        on_device, mesh=mesh, in_specs=in_specs, out_specs=out_specs, check_vma=False
    )
```

```python
import jax
import jax.numpy as jnp
from jax import lax
from jax.experimental import pallas as pl
from jax.experimental.pallas import tpu as pltpu
from jax.sharding import PartitionSpec as P

BLOCK = 64
LANES = 128


def entering_2(x, axis, combine, identity):
    count, index = (lax.axis_size(axis), lax.axis_index(axis))
    packed = lax.all_gather(jnp.stack(x), axis)
    before = identity
    for k in range(count):
        new = combine(before, (packed[k, 0], packed[k, 1]))
        reached = k < index
        before = jax.tree.map(lambda a, b: jnp.where(reached, a, b), new, before)
    return before


def from_behind(x, axis, by):
    count = lax.axis_size(axis)
    pairs = [(i, i + by) for i in range(count) if 0 <= i + by < count]
    return lax.ppermute(x, axis, pairs)


def combine_pairs(earlier, later):
    return (earlier[0] * later[0], later[0] * earlier[1] + later[1])


def expert_units(rows, gate_piece, up_piece):
    gate_pre = jnp.dot(rows, gate_piece, preferred_element_type=jnp.float32)
    up_pre = jnp.dot(rows, up_piece, preferred_element_type=jnp.float32)
    gate_cut = jnp.minimum(gate_pre, 7.0)
    up_cut = jnp.clip(up_pre, -7.0, 7.0)
    return ((up_cut + 1.0) * gate_cut * jax.nn.sigmoid(1.702 * gate_cut)).astype(jnp.bfloat16)


def down_product(units, down_pieces):
    total = None
    for part, piece in zip(units, down_pieces):
        term = lax.dot_general(
            part, piece, (((1,), (1,)), ((), ())), preferred_element_type=jnp.float32
        )
        total = term if total is None else total + term
    return total.astype(jnp.bfloat16)


def minus_expm1(v):
    series = 1.0 + v * (1.0 / 9.0)
    for n in range(8, 1, -1):
        series = 1.0 + v * (1.0 / n) * series
    return jnp.where(v > -0.5, -v * series, 1.0 - jnp.exp(v))


def mixer_kernel(
    behind_ref, source_ref, taps_ref, maps_ref, speeds_ref, spike_ref, state_ref, decay_ref
):
    channels, positions = source_ref.shape
    tap_count = taps_ref.shape[1]
    lane = lax.broadcasted_iota(jnp.int32, (channels, LANES), 1)

    def tile(index, carry):
        before, decay_in, state_in = carry
        here = pl.ds(pl.multiple_of(index * LANES, LANES), LANES)
        values = source_ref[:, here].astype(jnp.float32)
        running = None
        for tap in range(tap_count):
            back = tap_count - 1 - tap
            moved = values
            if back:
                moved = jnp.where(
                    lane >= back, pltpu.roll(values, back, 1), pltpu.roll(before, back, 1)
                )
            term = moved * taps_ref[:, tap : tap + 1]
            running = term if running is None else running + term
        conv_out = running.astype(jnp.bfloat16)
        both = jnp.dot(maps_ref[...], conv_out, preferred_element_type=jnp.float32)
        rate = 1.0 / (1.0 + jnp.exp(-both[:channels]))
        inflow = 1.0 / (1.0 + jnp.exp(-both[channels:]))
        exponent = -8.0 * rate * speeds_ref[...] + spike_ref[:, here]
        state = jnp.sqrt(minus_expm1(2.0 * exponent)) * inflow * conv_out.astype(jnp.float32)
        decay = jnp.exp(exponent)
        step = 1
        while step < LANES:
            inside = lane >= step
            state = decay * jnp.where(inside, pltpu.roll(state, step, 1), 0.0) + state
            decay = decay * jnp.where(inside, pltpu.roll(decay, step, 1), 1.0)
            step *= 2
        state = state + decay * state_in
        decay = decay * decay_in
        state_ref[:, here] = state
        decay_ref[:, here] = decay
        return values, decay[:, LANES - 1 :], state[:, LANES - 1 :]

    start = (
        behind_ref[...].astype(jnp.float32),
        jnp.ones((channels, 1), jnp.float32),
        jnp.zeros((channels, 1), jnp.float32),
    )
    lax.fori_loop(0, positions // LANES, tile, start)


def block_diagonal(maps):
    count, rows, columns = maps.shape
    same = jnp.eye(count, dtype=maps.dtype)
    spread = maps.transpose(0, 2, 1)[:, :, None, :] * same[:, None, :, None]
    return spread.reshape(count * columns, count * rows)


def mixer_half(
    scan_source_values,
    switch_path_values,
    causal_filter_coefficients,
    scan_switch_blockmap,
    entry_switch_blockmap,
    feature_fading_speeds,
    spike_amount,
    final_linear_map,
):
    channels, positions = scan_source_values.shape
    tp_index = lax.axis_index("tp")
    first_chan = tp_index * channels
    taps = lax.dynamic_slice_in_dim(causal_filter_coefficients, first_chan, channels, 0).astype(
        jnp.float32
    )
    behind = from_behind(scan_source_values[:, positions - LANES :], "ep", 1)
    block_count = channels // BLOCK
    maps = jnp.concatenate(
        [
            block_diagonal(lax.dynamic_slice_in_dim(m, tp_index * block_count, block_count, 0))
            for m in (scan_switch_blockmap, entry_switch_blockmap)
        ],
        axis=0,
    )
    speeds = lax.dynamic_slice_in_dim(feature_fading_speeds, first_chan, channels, 0)
    whole = jax.ShapeDtypeStruct((channels, positions), jnp.float32)
    local_state, local_decay = pl.pallas_call(
        mixer_kernel,
        out_shape=(whole, whole),
        in_specs=[pl.BlockSpec(memory_space=pltpu.VMEM)] * 6,
        out_specs=[pl.BlockSpec(memory_space=pltpu.VMEM)] * 2,
        compiler_params=pltpu.CompilerParams(vmem_limit_bytes=16 * 1024 * 1024),
        cost_estimate=pl.CostEstimate(
            flops=400 * channels * positions,
            bytes_accessed=10 * channels * positions,
            transcendentals=0,
        ),
    )(behind, scan_source_values, taps, maps, speeds[:, None], spike_amount[None, :])
    identity = (jnp.ones((channels,), jnp.float32), jnp.zeros((channels,), jnp.float32))
    carried = entering_2((local_decay[:, -1], local_state[:, -1]), "ep", combine_pairs, identity)
    state = local_state + local_decay * carried[1][:, None]
    mix_hidden = (
        state * jax.nn.gelu(switch_path_values.astype(jnp.float32), approximate=True)
    ).astype(jnp.bfloat16)
    tp_count = lax.axis_size("tp")
    pieces = mix_hidden.reshape(channels, tp_count, positions // tp_count)
    return lax.dot_general(
        lax.all_to_all(pieces, "tp", split_axis=1, concat_axis=0, tiled=True)[:, 0, :],
        final_linear_map,
        (((0,), (0,)), ((), ())),
        preferred_element_type=jnp.float32,
    ).astype(jnp.bfloat16)


def slot_places(ids, expert_count, slot_count):
    token_count = ids.shape[0]
    experts = jnp.arange(expert_count, dtype=jnp.int32)[None, None, :]
    named = (ids[:, :, None] == experts).astype(jnp.bfloat16)
    member = jnp.sum(named.astype(jnp.float32), axis=1).astype(jnp.bfloat16)
    order = jnp.arange(token_count, dtype=jnp.int32)
    earlier = (order[None, :] < order[:, None]).astype(jnp.bfloat16)
    rank = jnp.dot(earlier, member, preferred_element_type=jnp.float32)
    own_rank = jnp.sum(named.astype(jnp.float32) * rank[:, None, :], axis=2).astype(jnp.int32)
    return ids * slot_count + own_rank


def normed_rows(activity, gain):
    values = activity.astype(jnp.float32)
    scale = lax.rsqrt(jnp.mean(values * values, axis=1, keepdims=True) + 1e-06)
    return (values * scale * gain.astype(jnp.float32)).astype(jnp.bfloat16)


def rows_in_slots(rows, places, slot_total):
    slots = jnp.arange(slot_total, dtype=jnp.int32)[:, None]
    picks = slots == places[:, 0][None, :]
    for route in range(1, places.shape[1]):
        picks = picks | (slots == places[:, route][None, :])
    return jnp.dot(
        picks.astype(jnp.bfloat16), rows, preferred_element_type=jnp.float32
    ).astype(jnp.bfloat16)


def weighted_routes(returned, places, share):
    slots = jnp.arange(returned.shape[0], dtype=jnp.int32)[None, :]
    total = None
    for route in range(places.shape[1]):
        picks = (slots == places[:, route][:, None]).astype(jnp.bfloat16)
        chosen = jnp.dot(picks, returned, preferred_element_type=jnp.float32)
        term = chosen * share[:, route][:, None]
        total = term if total is None else total + term
    return total


def over_experts(rows, expert_count):
    width = rows.shape[1]
    pieces = rows.reshape(expert_count, rows.shape[0] // expert_count, width)
    return lax.all_to_all(pieces, "ep", split_axis=0, concat_axis=0, tiled=True).reshape(-1, width)


def expert_half(
    dispatched_group_activity,
    specialist_rmsgain,
    selected_specialist_ids,
    selected_specialist_share,
    specialist_switch_maps,
    specialist_widen_maps,
    specialist_shrink_maps,
):
    token_count, _ = dispatched_group_activity.shape
    route_count = selected_specialist_ids.shape[1]
    expert_count = lax.axis_size("ep")
    slot_count = 3 * route_count * token_count // (2 * expert_count)
    slot_total = expert_count * slot_count
    tp_count = lax.axis_size("tp")
    half = tp_count // 2
    swap = [(i, (i + half) % tp_count) for i in range(tp_count)]

    def half_pieces(piece):
        bit = half // 2
        while bit:
            other = lax.ppermute(piece, "tp", [(i, i ^ bit) for i in range(tp_count)])
            if bit == 1:
                return [piece, other]
            piece = jnp.concatenate([piece, other], axis=1)
            bit //= 2
        return [piece]

    table = jnp.concatenate(
        [selected_specialist_ids.astype(jnp.float32), selected_specialist_share], axis=1
    )
    far_table = lax.ppermute(table, "tp", swap)
    far_activity = lax.ppermute(dispatched_group_activity, "tp", swap)
    gate_pieces = half_pieces(specialist_switch_maps[0])
    up_pieces = half_pieces(specialist_widen_maps[0])
    down_pieces = half_pieces(specialist_shrink_maps[0])

    near_places = slot_places(selected_specialist_ids, expert_count, slot_count)
    near_normed = normed_rows(dispatched_group_activity, specialist_rmsgain)
    near_rows = rows_in_slots(near_normed, near_places, slot_total)
    near_arrived = over_experts(near_rows, expert_count)
    far_ids = far_table[:, :route_count].astype(jnp.int32)
    far_share = far_table[:, route_count:]
    far_places = slot_places(far_ids, expert_count, slot_count)
    far_rows = rows_in_slots(
        normed_rows(far_activity, specialist_rmsgain), far_places, slot_total
    )
    far_arrived = over_experts(far_rows, expert_count)
    arrived = jnp.concatenate([far_arrived, near_arrived], axis=0)
    units = [expert_units(arrived, g, u) for g, u in zip(gate_pieces, up_pieces)]
    far_result = down_product([part[:slot_total] for part in units], down_pieces)
    far_returned = over_experts(far_result, expert_count)
    near_result = down_product([part[slot_total:] for part in units], down_pieces)
    near_returned = over_experts(near_result, expert_count)
    far_sum = weighted_routes(far_returned, far_places, far_share).astype(jnp.bfloat16)
    home_sum = lax.ppermute(far_sum, "tp", swap)
    near_sum = weighted_routes(near_returned, near_places, selected_specialist_share)
    return (near_sum + home_sum.astype(jnp.float32)).astype(jnp.bfloat16)


def on_device(
    scan_source_values,
    switch_path_values,
    causal_filter_coefficients,
    scan_switch_blockmap,
    entry_switch_blockmap,
    feature_fading_speeds,
    spike_amount,
    final_linear_map,
    dispatched_group_activity,
    specialist_rmsgain,
    selected_specialist_ids,
    selected_specialist_share,
    specialist_switch_maps,
    specialist_widen_maps,
    specialist_shrink_maps,
):
    scan_path_result = mixer_half(
        scan_source_values,
        switch_path_values,
        causal_filter_coefficients,
        scan_switch_blockmap,
        entry_switch_blockmap,
        feature_fading_speeds,
        spike_amount,
        final_linear_map,
    )
    moe_out = expert_half(
        dispatched_group_activity,
        specialist_rmsgain,
        selected_specialist_ids,
        selected_specialist_share,
        specialist_switch_maps,
        specialist_widen_maps,
        specialist_shrink_maps,
    )
    return (scan_path_result, moe_out)


def solution(mesh):
    in_specs = (
        P("tp", "ep"),
        P("tp", "ep"),
        P(),
        P(),
        P(),
        P(),
        P("ep"),
        P(),
        P(("ep", "tp"), None),
        P(),
        P(("ep", "tp"), None),
        P(("ep", "tp"), None),
        P("ep", None, "tp"),
        P("ep", None, "tp"),
        P("ep", None, "tp"),
    )
    out_specs = (P(("ep", "tp"), None), P(("ep", "tp"), None))

    return jax.shard_map(
        on_device, mesh=mesh, in_specs=in_specs, out_specs=out_specs, check_vma=False
    )
```
